32 devices in a mesh: rep: 2 (over x), fs: 8 (over z, y), tp: 2 (over core).
Axes of the slice: x: 2, y: 2, z: 4, core: 2. Of those that a mesh axis runs over, the one named last changes fastest.
Arguments:
- tokens: bfloat16 [16, 192, 2048], P(('rep', 'fs'), 'tp'), may hold values from -6 to 6
- mix_gain: float32 [2048], replicated, may hold values from 0.1 to 1.9
- w_query: float32 [2048, 2048], P('fs', 'tp'), may hold values from -0.125 to 0.125
- w_key: float32 [2048, 2048], P('fs', 'tp'), may hold values from -0.125 to 0.125
- w_value: float32 [2048, 2048], P('fs', 'tp'), may hold values from -0.125 to 0.125
- w_out: float32 [2048, 2048], P('tp', 'fs'), may hold values from -0.125 to 0.125
- scale_query: float32 [2048], P('tp'), may hold values from 0.1 to 1.9
- scale_key: float32 [2048], P('tp'), may hold values from 0.1 to 1.9
- scale_value: float32 [2048], P('tp'), may hold values from 0.1 to 1.9
- scale_out: float32 [2048], replicated, may hold values from 0.1 to 1.9
- decay_rate: float32 [8], P('tp'), may hold values from 0.003 to 0.08
- mlp_gain: float32 [2048], replicated, may hold values from 0.1 to 1.9
- w_gate: float32 [2048, 3072], P('fs', 'tp'), may hold values from -0.125 to 0.125
- w_up: float32 [2048, 3072], P('fs', 'tp'), may hold values from -0.125 to 0.125
- w_down: float32 [3072, 2048], P('tp', 'fs'), may hold values from -0.109375 to 0.109375
- scale_gate: float32 [3072], P('tp'), may hold values from 0.1 to 1.9
- scale_up: float32 [3072], P('tp'), may hold values from 0.1 to 1.9
- scale_down: float32 [2048], replicated, may hold values from 0.1 to 1.9
Outputs:
- layer_out: bfloat16 [16, 192, 2048], P(('rep', 'fs'), 'tp')
The draws below stay inside these ranges and needn't reach their ends.
All inputs are finite; a program needn't handle non-finite values.
Results may differ from the reference program's by a relative error of at most 0.015.
Values may be sent and summed in bfloat16 or wider, within the bound.
A program may use at most 64 MiB of HBM per device.

```python
import math
import jax
import jax.numpy as jnp
from jax import lax

HEADS = 8
HEAD_DIM = 256
D = 2048
FF = 3072
BLOCK = 64
SEQ_LEN = 192
SEQS = 16
N_TP = 2


def shard_levels(rng, dims, cuts, least, high):
    level, own = 1.0, jax.random.fold_in(rng, 6)
    for axis_at, blocks in cuts:
        heights = jnp.exp(jax.random.uniform(jax.random.fold_in(own, axis_at), (blocks,), jnp.float32, least / len(cuts), high / len(cuts)))
        level = level * jnp.repeat(heights, dims[axis_at] // blocks).reshape([-1 if axis == axis_at else 1 for axis in range(len(dims))])
    return level


def noise(key, shape, deviation, reach, cuts=(), kind=jnp.bfloat16):
    values = deviation * jax.random.normal(key, shape, jnp.float32)
    if cuts:
        values = values * shard_levels(key, shape, cuts, -0.22, 0.18)
    return jnp.clip(values, -reach, reach).astype(kind)


def setup_inputs(seed: int = 0) -> dict:
    seeds = jax.random.split(jax.random.key(seed), 19)
    tokens = noise(seeds[0], (SEQS, SEQ_LEN, D), 1.0, 6.0, ((0, 16), (1, 2)))
    mix_gain = jnp.clip(1.0 + 0.18 * jax.random.normal(seeds[1], (D,), jnp.float32), 0.1, 1.9)
    w_query = noise(seeds[2], (D, D), D ** -0.5, 0.125, ((0, 8), (1, 2)), jnp.float32)
    w_key = noise(seeds[3], (D, D), D ** -0.5, 0.125, ((0, 8), (1, 2)), jnp.float32)
    w_value = noise(seeds[4], (D, D), D ** -0.5, 0.125, ((0, 8), (1, 2)), jnp.float32)
    w_out = noise(seeds[5], (D, D), D ** -0.5, 0.125, ((0, 2), (1, 8)), jnp.float32)
    scale_query = jnp.clip(1.0 + 0.18 * jax.random.normal(seeds[6], (D,), jnp.float32), 0.1, 1.9)
    scale_key = jnp.clip(1.0 + 0.18 * jax.random.normal(seeds[7], (D,), jnp.float32), 0.1, 1.9)
    scale_value = jnp.clip(1.0 + 0.18 * jax.random.normal(seeds[8], (D,), jnp.float32), 0.1, 1.9)
    scale_out = jnp.clip(1.0 + 0.18 * jax.random.normal(seeds[9], (D,), jnp.float32), 0.1, 1.9)
    decay_rate = jnp.clip(jnp.exp(math.log(0.08) - 3.2834143 * jax.random.uniform(seeds[10], (HEADS,), jnp.float32) ** shard_levels(seeds[10], (HEADS,), ((0, 2),), -0.2, 0.2)), 0.003, 0.08)
    mlp_gain = jnp.clip(1.0 + 0.18 * jax.random.normal(seeds[11], (D,), jnp.float32), 0.1, 1.9)
    w_gate = noise(seeds[12], (D, FF), D ** -0.5, 0.125, ((0, 8), (1, 2)), jnp.float32)
    w_up = noise(seeds[13], (D, FF), D ** -0.5, 0.125, ((0, 8), (1, 2)), jnp.float32)
    w_down = noise(seeds[14], (FF, D), FF ** -0.5, 0.109375, ((0, 2), (1, 8)), jnp.float32)
    scale_gate = jnp.clip(1.0 + 0.18 * jax.random.normal(seeds[15], (FF,), jnp.float32), 0.1, 1.9)
    scale_up = jnp.clip(1.0 + 0.18 * jax.random.normal(seeds[16], (FF,), jnp.float32), 0.1, 1.9)
    scale_down = jnp.clip(1.0 + 0.18 * jax.random.normal(seeds[17], (D,), jnp.float32), 0.1, 1.9)
    return dict(tokens=tokens, mix_gain=mix_gain, w_query=w_query, w_key=w_key, w_value=w_value, w_out=w_out, scale_query=scale_query, scale_key=scale_key, scale_value=scale_value, scale_out=scale_out, decay_rate=decay_rate, mlp_gain=mlp_gain, w_gate=w_gate, w_up=w_up, w_down=w_down, scale_gate=scale_gate, scale_up=scale_up, scale_down=scale_down)


EPS = 1e-06
ROPE_BASE = 10000.0

def rms_scale(values, gain):
    values = values.astype(jnp.float32)
    return values * lax.rsqrt(lax.optimization_barrier(jnp.mean(values * values, axis=-1, keepdims=True)) + EPS) * gain

def rotary(values, positions):
    width = values.shape[-1]
    half = width // 2
    inv_freq = 1.0 / ROPE_BASE ** (jnp.arange(0, width, 2, dtype=jnp.float32) / width)
    angles = positions.astype(jnp.float32)[:, None] * inv_freq[None, :]
    cosine = jnp.cos(angles)[:, None, :]
    sine = jnp.sin(angles)[:, None, :]
    first = values[..., :half]
    second = values[..., half:]
    return jnp.concatenate([first * cosine - second * sine, first * sine + second * cosine], axis=-1)

def retention(query, keyed, valued, rates):
    length, heads, width = query.shape
    nblocks = length // BLOCK

    def split(values):
        return values.reshape(nblocks, BLOCK, heads, width).transpose(0, 2, 1, 3)
    log_gamma = -rates
    inside = jnp.arange(BLOCK, dtype=jnp.float32)
    distance = inside[:, None] - inside[None, :]
    inner_product = jnp.where(distance[None] >= 0.0, jnp.exp(log_gamma[:, None, None] * jnp.maximum(distance, 0.0)[None]), 0.0)
    query_decay = jnp.exp(log_gamma[:, None] * (inside[None, :] + 1.0))
    key_decay_factor = jnp.exp(log_gamma[:, None] * (BLOCK - 1.0 - inside[None, :]))
    block_decay = jnp.exp(log_gamma * BLOCK)

    def advance(state, blocks):
        query_block_tile, key_block_tile, value_block_tile = blocks
        decay_weights = (jnp.einsum('frk,fvk->frv', query_block_tile.astype(jnp.float32), key_block_tile.astype(jnp.float32)) * inner_product).astype(jnp.bfloat16)
        local = jnp.einsum('hnm,hmv->hnv', decay_weights.astype(jnp.float32), value_block_tile.astype(jnp.float32))
        carried = jnp.einsum('hnd,hdv->hnv', query_block_tile.astype(jnp.float32) * query_decay[:, :, None], state, precision=lax.Precision.HIGHEST)
        state_update = jnp.einsum('asf,asp->afp', key_block_tile.astype(jnp.float32) * key_decay_factor[:, :, None], value_block_tile.astype(jnp.float32), precision=lax.Precision.HIGHEST)
        return (state * block_decay[:, None, None] + state_update, local + carried)
    initial = jnp.zeros((heads, width, width), jnp.float32)
    _, outs = lax.scan(advance, initial, (split(query), split(keyed), split(valued)))
    return outs.transpose(0, 2, 1, 3).reshape(length, heads, width)

def group_sum(inputs, weight, scale):
    length, inner_width = inputs.shape
    pieces = inputs.reshape(length, N_TP, inner_width // N_TP).astype(jnp.float32)
    blocks = weight.reshape(N_TP, inner_width // N_TP, weight.shape[1]).astype(jnp.float32)
    terms = jnp.einsum('ltc,tcd->ltd', pieces, blocks) * scale
    return lax.optimization_barrier(jnp.sum(terms.astype(jnp.bfloat16).astype(jnp.float32), axis=1))

def reference(tokens, mix_gain, w_query, w_key, w_value, w_out, scale_query, scale_key, scale_value, scale_out, decay_rate, mlp_gain, w_gate, w_up, w_down, scale_gate, scale_up, scale_down):
    query_w = w_query.astype(jnp.bfloat16)
    key_w = w_key.astype(jnp.bfloat16)
    value_w = w_value.astype(jnp.bfloat16)
    out_w = w_out.astype(jnp.bfloat16)
    gate_w = w_gate.astype(jnp.bfloat16)
    up_w = w_up.astype(jnp.bfloat16)
    down_w = w_down.astype(jnp.bfloat16)

    def one_sequence(rows):
        length = rows.shape[0]
        positions = jnp.arange(length)
        normed = rms_scale(rows, mix_gain).astype(jnp.bfloat16)
        query_raw = jnp.dot(normed, query_w, preferred_element_type=jnp.float32) * scale_query
        key_raw = jnp.dot(normed, key_w, preferred_element_type=jnp.float32) * scale_key
        value_raw = jnp.dot(normed, value_w, preferred_element_type=jnp.float32) * scale_value
        query_rows = rotary(query_raw.reshape(length, HEADS, HEAD_DIM), positions).astype(jnp.bfloat16)
        key_rows = rotary(key_raw.reshape(length, HEADS, HEAD_DIM), positions).astype(jnp.bfloat16)
        value_rows = value_raw.reshape(length, HEADS, HEAD_DIM).astype(jnp.bfloat16)
        retained = retention(query_rows, key_rows, value_rows, decay_rate)
        attended = rms_scale(retained, 1.0).astype(jnp.bfloat16).reshape(length, D)
        mixed = group_sum(attended, out_w, scale_out)
        hidden_state = (rows.astype(jnp.float32) + mixed).astype(jnp.bfloat16)
        mlp_in = rms_scale(hidden_state, mlp_gain).astype(jnp.bfloat16)
        gate_val = jnp.dot(mlp_in, gate_w, preferred_element_type=jnp.float32) * scale_gate
        up_val = jnp.dot(mlp_in, up_w, preferred_element_type=jnp.float32) * scale_up
        inner_product = (jax.nn.silu(gate_val) * up_val).astype(jnp.bfloat16)
        channel = group_sum(inner_product, down_w, scale_down)
        return (hidden_state.astype(jnp.float32) + channel).astype(jnp.bfloat16)
    return lax.map(one_sequence, tokens)
```

```python
import functools

import jax
import jax.numpy as jnp
from jax import lax
from jax.sharding import PartitionSpec as P

HEAD_DIM = 256

EPS = 1e-06
ROPE_BASE = 10000.0


def rms_scale(values, gain):
    values = values.astype(jnp.float32)
    return values * lax.rsqrt(jnp.mean(values * values, axis=-1, keepdims=True) + EPS) * gain


def rotary(values, positions):
    width = values.shape[-1]
    half = width // 2
    inv_freq = 1.0 / ROPE_BASE ** (jnp.arange(0, width, 2, dtype=jnp.float32) / width)
    angles = positions.astype(jnp.float32)[:, None] * inv_freq[None, :]
    cosine = jnp.cos(angles)[:, None, :]
    sine = jnp.sin(angles)[:, None, :]
    first = values[..., :half]
    second = values[..., half:]
    return jnp.concatenate(
        [first * cosine - second * sine, first * sine + second * cosine], axis=-1
    )


def retention(query, keyed, valued, rates):
    length = query.shape[1]
    place = jnp.arange(length, dtype=jnp.float32)
    distance = place[:, None] - place[None, :]
    decay = jnp.where(
        distance[None] >= 0.0,
        jnp.exp(-rates[:, None, None] * jnp.maximum(distance, 0.0)[None]),
        0.0,
    )
    scores = jnp.einsum("bnhd,bmhd->bhnm", query, keyed, preferred_element_type=jnp.float32)
    weights = (scores * decay[None]).astype(jnp.bfloat16)
    return jnp.einsum("bhnm,bmhv->bnhv", weights, valued, preferred_element_type=jnp.float32)


def per_device(
    reps,
    shards,
    halves,
    tokens,
    mix_gain,
    w_query,
    w_key,
    w_value,
    w_out,
    scale_query,
    scale_key,
    scale_value,
    scale_out,
    decay_rate,
    mlp_gain,
    w_gate,
    w_up,
    w_down,
    scale_gate,
    scale_up,
    scale_down,
):
    heads_tp = w_query.shape[1] // HEAD_DIM
    xs = 2 if reps == 2 and heads_tp % 2 == 0 else 1
    ys = 2 if shards % 2 == 0 and (heads_tp // xs) % 2 == 0 else 1
    team = xs * ys
    x = lax.axis_index("rep") if xs > 1 else 0
    fs_index = lax.axis_index("fs")
    y = fs_index % ys
    me = x * ys + y
    own_half = lax.axis_index("tp")

    def flip_chip(values, dx, dy):
        perm = []
        for r in range(reps):
            for f in range(shards):
                target_r = (r ^ 1) if dx else r
                target_f = (f ^ 1) if dy else f
                perm.append((r * shards + f, target_r * shards + target_f))
        return lax.ppermute(values, ("rep", "fs"), perm)

    offsets = [(dx, dy) for dx in range(xs) for dy in range(ys)]

    def cut(values, index, axis):
        size = values.shape[axis] // team
        return lax.dynamic_slice_in_dim(values, index * size, size, axis)

    def share(index, columned, rowed):
        parts = [cut(w, index, 1).astype(jnp.bfloat16) for w in columned]
        parts += [cut(w, index, 0).astype(jnp.bfloat16).T for w in rowed]
        return jnp.concatenate(parts, axis=1)

    def gather(columned, rowed):
        mine = share(me, columned, rowed)
        if ys > 1:
            theirs = flip_chip(share(x * ys + (1 - y), columned, rowed), 0, 1)
            first = jnp.where(y == 0, mine, theirs)
            second = jnp.where(y == 0, theirs, mine)
            mine = jnp.concatenate([first, second], axis=0)
        groups = [[s * ys + c for s in range(shards // ys)] for c in range(ys)]
        return lax.all_gather(mine, "fs", axis=0, tiled=True, axis_index_groups=groups)

    def gather_rows(rows):
        stacked = jnp.stack([flip_chip(rows, dx, dy) if dx or dy else rows for dx, dy in offsets])
        pieces = lax.all_gather(stacked, "tp", axis=1, tiled=True)
        return pieces.reshape(-1, rows.shape[-1])

    def scatter_rows(partial, rows):
        split = partial.astype(jnp.bfloat16).reshape(team, halves * rows, -1)
        if halves == 2:
            keep = lax.dynamic_slice_in_dim(split, own_half * rows, rows, 1)
            give = lax.dynamic_slice_in_dim(split, (1 - own_half) * rows, rows, 1)
            got = lax.ppermute(give, "tp", [(0, 1), (1, 0)])
            summed = keep.astype(jnp.float32) + got.astype(jnp.float32)
        else:
            summed = lax.psum_scatter(split, "tp", scatter_dimension=1, tiled=True)
            summed = summed.astype(jnp.float32)
        total = summed[0]
        for index, (dx, dy) in enumerate(offsets):
            if dx or dy:
                sent = flip_chip(summed[index].astype(jnp.bfloat16), dx, dy)
                total = total + sent.astype(jnp.float32)
        return total

    own_rows = tokens[0]
    rows = own_rows.shape[0]
    length = rows * halves
    normed = gather_rows(rms_scale(own_rows, mix_gain).astype(jnp.bfloat16))
    mixer = gather((w_query, w_key, w_value), (w_out,))
    width = w_query.shape[1] // team
    heads_here = width // HEAD_DIM
    raw = jnp.dot(normed, mixer[:, : 3 * width], preferred_element_type=jnp.float32)
    positions = jnp.arange(length)

    def heads_of(index, scale):
        values = raw[:, index * width : (index + 1) * width] * cut(scale, me, 0)
        return values.reshape(team, length, heads_here, HEAD_DIM)

    query = rotary(heads_of(0, scale_query), positions).astype(jnp.bfloat16)
    keyed = rotary(heads_of(1, scale_key), positions).astype(jnp.bfloat16)
    valued = heads_of(2, scale_value).astype(jnp.bfloat16)
    retained = retention(query, keyed, valued, cut(decay_rate, me, 0))
    attended = rms_scale(retained, 1.0).astype(jnp.bfloat16).reshape(team * length, width)
    contract = (((1,), (1,)), ((), ()))
    partial = (
        lax.dot_general(
            attended, mixer[:, 3 * width :], contract, preferred_element_type=jnp.float32
        )
        * scale_out
    )
    mixed = scatter_rows(partial, rows)
    hidden_state = (own_rows.astype(jnp.float32) + mixed).astype(jnp.bfloat16)
    mlp_in = gather_rows(rms_scale(hidden_state, mlp_gain).astype(jnp.bfloat16))
    channel_mixer = gather((w_gate, w_up), (w_down,))
    units = w_gate.shape[1] // team
    both = jnp.dot(mlp_in, channel_mixer[:, : 2 * units], preferred_element_type=jnp.float32)
    gate_val = both[:, :units] * cut(scale_gate, me, 0)
    up_val = both[:, units:] * cut(scale_up, me, 0)
    inner = (jax.nn.silu(gate_val) * up_val).astype(jnp.bfloat16)
    partial = (
        lax.dot_general(
            inner, channel_mixer[:, 2 * units :], contract, preferred_element_type=jnp.float32
        )
        * scale_down
    )
    channel = scatter_rows(partial, rows)
    return (hidden_state.astype(jnp.float32) + channel).astype(jnp.bfloat16)[None]


def solution(mesh):
    in_specs = (
        P(("rep", "fs"), "tp", None),
        P(),
        P("fs", "tp"),
        P("fs", "tp"),
        P("fs", "tp"),
        P("tp", "fs"),
        P("tp"),
        P("tp"),
        P("tp"),
        P(),
        P("tp"),
        P(),
        P("fs", "tp"),
        P("fs", "tp"),
        P("tp", "fs"),
        P("tp"),
        P("tp"),
        P(),
    )
    out_specs = P(("rep", "fs"), "tp", None)
    body = functools.partial(
        per_device, mesh.shape["rep"], mesh.shape["fs"], mesh.shape["tp"]
    )
    return jax.shard_map(
        body, mesh=mesh, in_specs=in_specs, out_specs=out_specs, check_vma=False
    )
```

```python
import functools

import jax
import jax.numpy as jnp
from jax import lax
from jax.sharding import PartitionSpec as P

HEAD_DIM = 256


EPS = 1e-06
ROPE_BASE = 10000.0


def rms_scale(values, gain):
    values = values.astype(jnp.float32)
    return values * lax.rsqrt(jnp.mean(values * values, axis=-1, keepdims=True) + EPS) * gain


def rotary(values, positions):
    width = values.shape[-1]
    half = width // 2
    inv_freq = 1.0 / ROPE_BASE ** (jnp.arange(0, width, 2, dtype=jnp.float32) / width)
    angles = positions.astype(jnp.float32)[:, None] * inv_freq[None, :]
    cosine = jnp.cos(angles)[:, None, :]
    sine = jnp.sin(angles)[:, None, :]
    first = values[..., :half]
    second = values[..., half:]
    return jnp.concatenate(
        [first * cosine - second * sine, first * sine + second * cosine], axis=-1
    )


def retention(query, keyed, valued, rates):
    length = query.shape[1]
    place = jnp.arange(length, dtype=jnp.float32)
    distance = place[:, None] - place[None, :]
    decay = jnp.where(
        distance[None] >= 0.0,
        jnp.exp(-rates[:, None, None] * jnp.maximum(distance, 0.0)[None]),
        0.0,
    )
    scores = jnp.einsum("bnhd,bmhd->bhnm", query, keyed, preferred_element_type=jnp.float32)
    weights = (scores * decay[None]).astype(jnp.bfloat16)
    return jnp.einsum("bhnm,bmhv->bnhv", weights, valued, preferred_element_type=jnp.float32)


def per_device(
    reps,
    shards,
    halves,
    tokens,
    mix_gain,
    w_query,
    w_key,
    w_value,
    w_out,
    scale_query,
    scale_key,
    scale_value,
    scale_out,
    decay_rate,
    mlp_gain,
    w_gate,
    w_up,
    w_down,
    scale_gate,
    scale_up,
    scale_down,
):
    heads_tp = w_query.shape[1] // HEAD_DIM
    xs = 2 if reps == 2 and heads_tp % 2 == 0 else 1
    ys = 2 if shards % 2 == 0 and (heads_tp // xs) % 2 == 0 else 1
    team = xs * ys
    x = lax.axis_index("rep") if xs > 1 else 0
    fs_index = lax.axis_index("fs")
    y = fs_index % ys
    me = x * ys + y
    own_half = lax.axis_index("tp")

    def flip_chip(values, dx, dy):
        perm = []
        for r in range(reps):
            for f in range(shards):
                target_r = (r ^ 1) if dx else r
                target_f = (f ^ 1) if dy else f
                perm.append((r * shards + f, target_r * shards + target_f))
        return lax.ppermute(values, ("rep", "fs"), perm)

    offsets = [(dx, dy) for dx in range(xs) for dy in range(ys)]

    def cut(values, index, axis):
        size = values.shape[axis] // team
        return lax.dynamic_slice_in_dim(values, index * size, size, axis)

    def share(index, columned, rowed):
        parts = [cut(w, index, 1).astype(jnp.bfloat16) for w in columned]
        parts += [cut(w, index, 0).astype(jnp.bfloat16).T for w in rowed]
        return jnp.concatenate(parts, axis=1)

    groups = [[s * ys + c for s in range(shards // ys)] for c in range(ys)]

    def along(values):
        return lax.all_gather(values, "fs", axis=0, tiled=True, axis_index_groups=groups)

    def swapped(columned, rowed):
        return flip_chip(share(x * ys + (1 - y), columned, rowed), 0, 1)

    def by_y(mine, theirs):
        return [jnp.where(y == 0, mine, theirs), jnp.where(y == 0, theirs, mine)]

    def gather_rows(rows):
        stacked = jnp.stack([flip_chip(rows, dx, dy) if dx or dy else rows for dx, dy in offsets])
        if halves == 2:
            other = lax.ppermute(stacked, "tp", [(0, 1), (1, 0)])
            first = jnp.where(own_half == 0, stacked, other)
            second = jnp.where(own_half == 0, other, stacked)
            pieces = jnp.concatenate([first, second], axis=1)
        else:
            pieces = lax.all_gather(stacked, "tp", axis=1, tiled=True)
        return pieces.reshape(-1, rows.shape[-1])

    def scatter_rows(partial, rows):
        split = partial.astype(jnp.bfloat16).reshape(team, halves * rows, -1)
        if halves == 2:
            keep = lax.dynamic_slice_in_dim(split, own_half * rows, rows, 1)
            give = lax.dynamic_slice_in_dim(split, (1 - own_half) * rows, rows, 1)
            got = lax.ppermute(give, "tp", [(0, 1), (1, 0)])
            summed = keep.astype(jnp.float32) + got.astype(jnp.float32)
        else:
            summed = lax.psum_scatter(split, "tp", scatter_dimension=1, tiled=True)
            summed = summed.astype(jnp.float32)
        total = summed[0]
        for index, (dx, dy) in enumerate(offsets):
            if dx or dy:
                sent = flip_chip(summed[index].astype(jnp.bfloat16), dx, dy)
                total = total + sent.astype(jnp.float32)
        return total

    own_rows = tokens[0]
    rows = own_rows.shape[0]
    length = rows * halves
    width = w_query.shape[1] // team
    heads_here = width // HEAD_DIM
    mixing = ((w_query, w_key, w_value), (w_out,))
    channeling = ((w_gate, w_up), (w_down,))
    mixer = along(share(me, *mixing))
    normed_own = rms_scale(own_rows, mix_gain).astype(jnp.bfloat16)
    if ys > 1:
        mixer_swap = swapped(*mixing)
        channel_swap = swapped(*channeling)
        channel_own = share(me, *channeling)
        channel_pair = jnp.concatenate(by_y(channel_own, channel_swap), axis=0)
        normed_own, mixer_swap = lax.optimization_barrier((normed_own, mixer_swap))
        mixer_other = along(mixer_swap)
        normed = gather_rows(normed_own)
        normed, channel_pair = lax.optimization_barrier((normed, channel_pair))
        channel_mixer = along(channel_pair)
        pieces = normed.reshape(team * length, shards // ys, ys, -1)
        own_part, other_part = by_y(pieces[:, :, 0], pieces[:, :, 1])
        raw = jnp.dot(
            own_part.reshape(team * length, -1),
            mixer[:, : 3 * width],
            preferred_element_type=jnp.float32,
        ) + jnp.dot(
            other_part.reshape(team * length, -1),
            mixer_other[:, : 3 * width],
            preferred_element_type=jnp.float32,
        )
        pair = by_y(mixer[:, 3 * width :], mixer_other[:, 3 * width :])
        cut_rows = [part.reshape(shards // ys, -1, width) for part in pair]
        out_rows = jnp.stack(cut_rows, axis=1).reshape(-1, width)
    else:
        channel_mixer = along(share(me, *channeling))
        normed = gather_rows(normed_own)
        raw = jnp.dot(normed, mixer[:, : 3 * width], preferred_element_type=jnp.float32)
        out_rows = mixer[:, 3 * width :]
    positions = jnp.arange(length)

    def heads_of(index, scale):
        values = raw[:, index * width : (index + 1) * width] * cut(scale, me, 0)
        return values.reshape(team, length, heads_here, HEAD_DIM)

    query = rotary(heads_of(0, scale_query), positions).astype(jnp.bfloat16)
    keyed = rotary(heads_of(1, scale_key), positions).astype(jnp.bfloat16)
    valued = heads_of(2, scale_value).astype(jnp.bfloat16)
    retained = retention(query, keyed, valued, cut(decay_rate, me, 0))
    attended = rms_scale(retained, 1.0).astype(jnp.bfloat16).reshape(team * length, width)
    contract = (((1,), (1,)), ((), ()))
    partial = (
        lax.dot_general(
            attended, out_rows, contract, preferred_element_type=jnp.float32
        )
        * scale_out
    )
    mixed = scatter_rows(partial, rows)
    hidden_state = (own_rows.astype(jnp.float32) + mixed).astype(jnp.bfloat16)
    mlp_in = gather_rows(rms_scale(hidden_state, mlp_gain).astype(jnp.bfloat16))
    units = w_gate.shape[1] // team
    both = jnp.dot(mlp_in, channel_mixer[:, : 2 * units], preferred_element_type=jnp.float32)
    gate_val = both[:, :units] * cut(scale_gate, me, 0)
    up_val = both[:, units:] * cut(scale_up, me, 0)
    inner = (jax.nn.silu(gate_val) * up_val).astype(jnp.bfloat16)
    partial = (
        lax.dot_general(
            inner, channel_mixer[:, 2 * units :], contract, preferred_element_type=jnp.float32
        )
        * scale_down
    )
    channel = scatter_rows(partial, rows)
    return (hidden_state.astype(jnp.float32) + channel).astype(jnp.bfloat16)[None]


def solution(mesh):
    in_specs = (
        P(("rep", "fs"), "tp", None),
        P(),
        P("fs", "tp"),
        P("fs", "tp"),
        P("fs", "tp"),
        P("tp", "fs"),
        P("tp"),
        P("tp"),
        P("tp"),
        P(),
        P("tp"),
        P(),
        P("fs", "tp"),
        P("fs", "tp"),
        P("tp", "fs"),
        P("tp"),
        P("tp"),
        P(),
    )
    out_specs = P(("rep", "fs"), "tp", None)
    body = functools.partial(
        per_device, mesh.shape["rep"], mesh.shape["fs"], mesh.shape["tp"]
    )
    return jax.shard_map(
        body, mesh=mesh, in_specs=in_specs, out_specs=out_specs, check_vma=False
    )
```

```python
import functools

import jax
import jax.numpy as jnp
from jax import lax
from jax.sharding import PartitionSpec as P

HEAD_DIM = 256


EPS = 1e-06
ROPE_BASE = 10000.0


def rms_scale(values, gain):
    values = values.astype(jnp.float32)
    return values * lax.rsqrt(jnp.mean(values * values, axis=-1, keepdims=True) + EPS) * gain


def rotary(values, positions):
    width = values.shape[-1]
    half = width // 2
    inv_freq = 1.0 / ROPE_BASE ** (jnp.arange(0, width, 2, dtype=jnp.float32) / width)
    angles = positions.astype(jnp.float32)[:, None] * inv_freq[None, :]
    cosine = jnp.cos(angles)[:, None, :]
    sine = jnp.sin(angles)[:, None, :]
    first = values[..., :half]
    second = values[..., half:]
    return jnp.concatenate(
        [first * cosine - second * sine, first * sine + second * cosine], axis=-1
    )


def retention(query, keyed, valued, rates):
    length = query.shape[1]
    place = jnp.arange(length, dtype=jnp.float32)
    distance = place[:, None] - place[None, :]
    decay = jnp.where(
        distance[None] >= 0.0,
        jnp.exp(-rates[:, None, None] * jnp.maximum(distance, 0.0)[None]),
        0.0,
    )
    scores = jnp.einsum("bnhd,bmhd->bhnm", query, keyed, preferred_element_type=jnp.float32)
    weights = (scores * decay[None]).astype(jnp.bfloat16)
    return jnp.einsum("bhnm,bmhv->bnhv", weights, valued, preferred_element_type=jnp.float32)


def per_device(
    reps,
    shards,
    halves,
    tokens,
    mix_gain,
    w_query,
    w_key,
    w_value,
    w_out,
    scale_query,
    scale_key,
    scale_value,
    scale_out,
    decay_rate,
    mlp_gain,
    w_gate,
    w_up,
    w_down,
    scale_gate,
    scale_up,
    scale_down,
):
    heads_tp = w_query.shape[1] // HEAD_DIM
    xs = 2 if reps == 2 and heads_tp % 2 == 0 else 1
    ys = 2 if shards % 2 == 0 and (heads_tp // xs) % 2 == 0 else 1
    team = xs * ys
    x = lax.axis_index("rep") if xs > 1 else 0
    fs_index = lax.axis_index("fs")
    y = fs_index % ys
    me = x * ys + y
    own_half = lax.axis_index("tp")

    def flip_chip(values, dx, dy):
        perm = []
        for r in range(reps):
            for f in range(shards):
                target_r = (r ^ 1) if dx else r
                target_f = (f ^ 1) if dy else f
                perm.append((r * shards + f, target_r * shards + target_f))
        return lax.ppermute(values, ("rep", "fs"), perm)

    offsets = [(dx, dy) for dx in range(xs) for dy in range(ys)]

    def cut(values, index, axis):
        size = values.shape[axis] // team
        return lax.dynamic_slice_in_dim(values, index * size, size, axis)

    def share(index, columned, rowed):
        parts = [cut(w, index, 1).astype(jnp.bfloat16) for w in columned]
        parts += [cut(w, index, 0).astype(jnp.bfloat16).T for w in rowed]
        return jnp.concatenate(parts, axis=1)

    groups = [[s * ys + c for s in range(shards // ys)] for c in range(ys)]

    def along(values):
        return lax.all_gather(values, "fs", axis=0, tiled=True, axis_index_groups=groups)

    def swapped(columned, rowed):
        return flip_chip(share(x * ys + (1 - y), columned, rowed), 0, 1)

    def hop_along(values):
        lines = shards // ys
        size = values.shape[0]
        line = fs_index // ys
        whole = jnp.zeros((lines * size, values.shape[1]), values.dtype)
        for step in range(lines):
            block = values
            if step:
                perm = [(f, (f + step * ys) % shards) for f in range(shards)]
                block = lax.ppermute(values, "fs", perm)
            source = (line + lines - step) % lines
            whole = lax.dynamic_update_slice(whole, block, (source * size, 0))
        return whole

    def by_y(mine, theirs):
        return [jnp.where(y == 0, mine, theirs), jnp.where(y == 0, theirs, mine)]

    def gather_rows(rows):
        stacked = jnp.stack([flip_chip(rows, dx, dy) if dx or dy else rows for dx, dy in offsets])
        if halves == 2:
            other = lax.ppermute(stacked, "tp", [(0, 1), (1, 0)])
            first = jnp.where(own_half == 0, stacked, other)
            second = jnp.where(own_half == 0, other, stacked)
            pieces = jnp.concatenate([first, second], axis=1)
        else:
            pieces = lax.all_gather(stacked, "tp", axis=1, tiled=True)
        return pieces.reshape(-1, rows.shape[-1])

    def scatter_rows(partial, rows):
        split = partial.astype(jnp.bfloat16).reshape(team, halves * rows, -1)
        if halves == 2:
            keep = lax.dynamic_slice_in_dim(split, own_half * rows, rows, 1)
            give = lax.dynamic_slice_in_dim(split, (1 - own_half) * rows, rows, 1)
            got = lax.ppermute(give, "tp", [(0, 1), (1, 0)])
            summed = keep.astype(jnp.float32) + got.astype(jnp.float32)
        else:
            summed = lax.psum_scatter(split, "tp", scatter_dimension=1, tiled=True)
            summed = summed.astype(jnp.float32)
        total = summed[0]
        for index, (dx, dy) in enumerate(offsets):
            if dx or dy:
                sent = flip_chip(summed[index].astype(jnp.bfloat16), dx, dy)
                total = total + sent.astype(jnp.float32)
        return total

    own_rows = tokens[0]
    rows = own_rows.shape[0]
    length = rows * halves
    width = w_query.shape[1] // team
    heads_here = width // HEAD_DIM
    mixing = ((w_query, w_key, w_value), (w_out,))
    channeling = ((w_gate, w_up), (w_down,))
    mixer = along(share(me, *mixing))
    normed_own = rms_scale(own_rows, mix_gain).astype(jnp.bfloat16)
    if ys > 1:
        mixer_swap = swapped(*mixing)
        channel_swap = swapped(*channeling)
        channel_own = share(me, *channeling)
        channel_pair = jnp.concatenate(by_y(channel_own, channel_swap), axis=0)
        normed_own, mixer_swap = lax.optimization_barrier((normed_own, mixer_swap))
        mixer_other = along(mixer_swap)
        normed = gather_rows(normed_own)
        normed, channel_pair = lax.optimization_barrier((normed, channel_pair))
        split = channel_pair.shape[1] - w_down.shape[0] // team
        channel_mixer = along(channel_pair[:, :split])
        down_rows = hop_along(channel_pair[:, split:])
        pieces = normed.reshape(team * length, shards // ys, ys, -1)
        own_part, other_part = by_y(pieces[:, :, 0], pieces[:, :, 1])
        other_part, down_rows = lax.optimization_barrier((other_part, down_rows))
        raw = jnp.dot(
            own_part.reshape(team * length, -1),
            mixer[:, : 3 * width],
            preferred_element_type=jnp.float32,
        ) + jnp.dot(
            other_part.reshape(team * length, -1),
            mixer_other[:, : 3 * width],
            preferred_element_type=jnp.float32,
        )
        pair = by_y(mixer[:, 3 * width :], mixer_other[:, 3 * width :])
        cut_rows = [part.reshape(shards // ys, -1, width) for part in pair]
        out_rows = jnp.stack(cut_rows, axis=1).reshape(-1, width)
    else:
        channel_mixer = along(share(me, *channeling))
        normed = gather_rows(normed_own)
        raw = jnp.dot(normed, mixer[:, : 3 * width], preferred_element_type=jnp.float32)
        out_rows = mixer[:, 3 * width :]
        down_rows = channel_mixer[:, 2 * (w_gate.shape[1] // team) :]
    positions = jnp.arange(length)

    def heads_of(index, scale):
        values = raw[:, index * width : (index + 1) * width] * cut(scale, me, 0)
        return values.reshape(team, length, heads_here, HEAD_DIM)

    query = rotary(heads_of(0, scale_query), positions).astype(jnp.bfloat16)
    keyed = rotary(heads_of(1, scale_key), positions).astype(jnp.bfloat16)
    valued = heads_of(2, scale_value).astype(jnp.bfloat16)
    retained = retention(query, keyed, valued, cut(decay_rate, me, 0))
    attended = rms_scale(retained, 1.0).astype(jnp.bfloat16).reshape(team * length, width)
    contract = (((1,), (1,)), ((), ()))
    partial = (
        lax.dot_general(
            attended, out_rows, contract, preferred_element_type=jnp.float32
        )
        * scale_out
    )
    mixed = scatter_rows(partial, rows)
    hidden_state = (own_rows.astype(jnp.float32) + mixed).astype(jnp.bfloat16)
    mlp_in = gather_rows(rms_scale(hidden_state, mlp_gain).astype(jnp.bfloat16))
    units = w_gate.shape[1] // team
    both = jnp.dot(mlp_in, channel_mixer[:, : 2 * units], preferred_element_type=jnp.float32)
    gate_val = both[:, :units] * cut(scale_gate, me, 0)
    up_val = both[:, units:] * cut(scale_up, me, 0)
    inner = (jax.nn.silu(gate_val) * up_val).astype(jnp.bfloat16)
    partial = (
        lax.dot_general(
            inner, down_rows, contract, preferred_element_type=jnp.float32
        )
        * scale_down
    )
    channel = scatter_rows(partial, rows)
    return (hidden_state.astype(jnp.float32) + channel).astype(jnp.bfloat16)[None]


def solution(mesh):
    in_specs = (
        P(("rep", "fs"), "tp", None),
        P(),
        P("fs", "tp"),
        P("fs", "tp"),
        P("fs", "tp"),
        P("tp", "fs"),
        P("tp"),
        P("tp"),
        P("tp"),
        P(),
        P("tp"),
        P(),
        P("fs", "tp"),
        P("fs", "tp"),
        P("tp", "fs"),
        P("tp"),
        P("tp"),
        P(),
    )
    out_specs = P(("rep", "fs"), "tp", None)
    body = functools.partial(
        per_device, mesh.shape["rep"], mesh.shape["fs"], mesh.shape["tp"]
    )
    return jax.shard_map(
        body, mesh=mesh, in_specs=in_specs, out_specs=out_specs, check_vma=False
    )
```
